128 devices in a mesh: ep: 32 (over z, y, core), tp: 4 (over x).
Axes of the slice: x: 4, y: 4, z: 4, core: 2. Of those that a mesh axis runs over, the one named last changes fastest.
Arguments:
- tokens: bfloat16 [10240, 2048], P('ep'), may hold values from -12 to 12, as said below
- cotangent: bfloat16 [10240, 2048], P('ep'), may hold values from -0.59765625 to 0.59765625
- route_ids: int32 [10240, 2], P('ep'), may hold values from 0 to 31, all different within a row; in each aligned block of 320 rows (0 to 319, 320 to 639, ...) at most 40 rows name the same one
- route_weights: bfloat16 [10240, 2], P('ep'), may hold values from 0.049804688 to 1
- w_gate: bfloat16 [32, 2048, 2048], P('ep', None, 'tp'), may hold values from -0.125 to 0.125
- w_up: bfloat16 [32, 2048, 2048], P('ep', None, 'tp'), may hold values from -0.125 to 0.125
- w_down: bfloat16 [32, 2048, 2048], P('ep', 'tp'), may hold values from -0.125 to 0.125
- dense_in: bfloat16 [2048, 256], P(('ep', 'tp')), may hold values from -0.125 to 0.125
- dense_out: bfloat16 [2048, 256], P(('ep', 'tp')), may hold values from -0.375 to 0.375
- dense_gate: bfloat16 [2048], replicated, may hold values from -0.125 to 0.125
Outputs:
- grad_tokens: bfloat16 [10240, 2048], P('ep', 'tp')
- grad_route_weights: bfloat16 [10240, 2], P('ep')
- grad_gate: float32 [32, 2048, 2048], P('ep', None, 'tp')
- grad_up: float32 [32, 2048, 2048], P('ep', None, 'tp')
- grad_down: float32 [32, 2048, 2048], P('ep', 'tp')
- grad_dense_in: float32 [2048, 256], P(('ep', 'tp'))
- grad_dense_out: float32 [2048, 256], P(('ep', 'tp'))
- grad_dense_gate: float32 [2048], P(('ep', 'tp'))
The draws below stay inside these ranges and needn't reach their ends.
Inputs may be any that keep to these rules, and one draw needn't show every extreme that they name: `route_ids`: each row names 2 different experts; among the rows of one index of ep no expert is named more than 40 times, and that count is reached. `tokens`: rows carry scales between 0.5 and 2 that differ from row to row.
All inputs are finite; a program needn't handle non-finite values.
Results may differ from the reference program's by a relative error of at most 0.01.
Values may be sent and summed in bfloat16 or wider, within the bound.
No kernel may reach another device: no remote copies, remote signals or barrier semaphores. Data moves between devices by JAX's collectives and lax.ppermute only.
A program may use at most 128 MiB of HBM per device.

```python
import math
import jax
import jax.numpy as jnp
import numpy as np
from jax import lax

D = 2048
FF = 2048
R = 256
TOP = 2
TOK_DEV = 320
EXPERTS = 32
CAP = 40
TOKENS = 10240
N_EP = 32
N_TP = 4


def draw_tokens(key, part):
    base_key = jax.random.fold_in(key, 11)
    scale_key = jax.random.fold_in(key, 12)
    scales = jnp.exp(jax.random.uniform(scale_key, (TOKENS, 1), jnp.float32, math.log(0.5), math.log(2.0)))
    base = jax.random.normal(base_key, (TOKENS, D), jnp.float32)
    base = jnp.clip(base, -6.0, 6.0)
    return (base * scales).astype(jnp.bfloat16)


def levels(own_key, extent, pieces, low, top_value):
    def one(dim, blocks):
        draws = jax.random.uniform(jax.random.fold_in(jax.random.fold_in(own_key, 6), dim), (blocks,), jnp.float32, low / len(pieces), top_value / len(pieces))
        return jnp.repeat(jnp.exp(draws), extent[dim] // blocks).reshape((-1,) + (1,) * (len(extent) - dim - 1))

    loudness = one(*pieces[0])
    for cut in pieces[1:]:
        loudness = loudness * one(*cut)
    return loudness


def routed_block(rng, own, number, rows, number_of, top, limit, slope):
    order = jax.random.permutation(rng, number_of)
    crowded, common = shares(number_of, rows * top, limit, slope, True), shares(number_of, rows * top, limit, slope, False)
    places = jnp.arange(number_of)

    def named(lengths, offset_by):
        used = int((lengths > 0).sum())
        fixed = max(1, used // 4)
        passed = fixed + (places - fixed + offset_by * (used - fixed)) % max(1, number_of - fixed)
        return jnp.zeros((number_of,), jnp.int32).at[order[jnp.where(places < fixed, places, passed)]].set(jnp.asarray(lengths, jnp.int32))

    lengths = jnp.where(number % 4 == 0, named(crowded, number // 4), named(common, number - number // 4 - 1))
    mixed = jax.random.permutation(jax.random.fold_in(own, 3), number_of)
    giver, receiver = mixed[0:number_of // 2 * 2:2], mixed[1:number_of // 2 * 2:2]
    margin = jnp.minimum(lengths[giver] - 1, limit - lengths[receiver]) // 2
    margin = jnp.where((giver == order[0]) | (receiver == order[0]) | (lengths[receiver] == 0), 0, jnp.maximum(margin, 0))
    passed = jax.random.randint(jax.random.fold_in(own, 4), (number_of // 2,), 0, 1 << 20) % (margin + 1)
    lengths = lengths.at[giver].add(-passed).at[receiver].add(passed)
    items = jnp.searchsorted(jnp.cumsum(lengths), jnp.arange(rows * top), side="right").astype(jnp.int32)
    grid = items.reshape(top, rows).T
    grid = grid[jax.random.permutation(jax.random.fold_in(own, 1), rows)]
    offset_by = jax.random.randint(jax.random.fold_in(own, 2), (rows, 1), 0, top)
    return jnp.take_along_axis(grid, (jnp.arange(top)[None, :] + offset_by) % top, axis=1)


def shares(amount, total, limit, skew, full):
    weights = [(1 << 20) // math.isqrt(rank ** skew) + 1 for rank in range(1, amount + 1)]
    largest = limit if full else min(limit, max(-(-total // amount), total * weights[0] // sum(weights)))
    least = 1 if total - largest >= amount - 1 else 0
    given, rest = [largest] + [least] * (amount - 1), total - largest - least * (amount - 1)
    while rest > 0:
        free = [i for i in range(1, amount) if given[i] < largest] or [i for i in range(1, amount) if given[i] < limit]
        whole, left = sum([weights[i] for i in free]), rest
        for i in free:
            extra = min(limit - given[i], max(1, left * weights[i] // whole), rest)
            given[i] = given[i] + extra
            rest = rest - extra
    return np.array(given)


def scatter_about(stream_key, shape, deviation, most, split=(), kind=jnp.bfloat16):
    values = jax.random.normal(stream_key, shape, jnp.float32) * deviation
    if len(split) > 0:
        values = levels(stream_key, shape, split, -0.22, 0.18) * values
    return jnp.clip(values, min=-most, max=most).astype(kind)


def setup_inputs(seed: int = 0) -> dict:
    keys = jax.random.split(jax.random.key(seed), 11)
    tokens = draw_tokens(jax.random.fold_in(keys[10], 71), 0)
    cotangent = scatter_about(keys[1], (TOKENS, D), 0.1, 0.59765625, ((0, 32),))
    route_ids_keys = jax.random.split(jax.random.fold_in(keys[2], 1), TOKENS // TOK_DEV)
    route_ids_turns = jax.random.permutation(jax.random.fold_in(keys[2], 3), TOKENS // TOK_DEV)
    route_ids = jax.vmap(lambda own, number: routed_block(jax.random.fold_in(keys[2], 2), own, number, TOK_DEV, EXPERTS, TOP, CAP, 2))(route_ids_keys, route_ids_turns).reshape((TOKENS, TOP))
    route_weights = jnp.clip(0.049804688 + 0.9501953 * jax.random.uniform(keys[3], (TOKENS, TOP), jnp.float32) ** levels(keys[3], (TOKENS, TOP), ((0, 32),), -0.2, 0.2), 0.049804688, 1.0).astype(jnp.bfloat16)
    w_gate = scatter_about(keys[4], (EXPERTS, D, FF), D ** -0.5, 0.125, ((0, 32), (2, 4)))
    w_up = scatter_about(keys[5], (EXPERTS, D, FF), D ** -0.5, 0.125, ((0, 32), (2, 4)))
    w_down = scatter_about(keys[6], (EXPERTS, FF, D), FF ** -0.5, 0.125, ((0, 32), (1, 4)))
    dense_in = scatter_about(keys[7], (D, R), D ** -0.5, 0.125, ((0, 128),))
    dense_out = scatter_about(keys[8], (D, R), R ** -0.5, 0.375, ((0, 128),))
    dense_gate = scatter_about(keys[9], (D,), D ** -0.5, 0.125)
    return dict(tokens=tokens, cotangent=cotangent, route_ids=route_ids, route_weights=route_weights, w_gate=w_gate, w_up=w_up, w_down=w_down, dense_in=dense_in, dense_out=dense_out, dense_gate=dense_gate)


CLAMP_LIMIT = 7.0
SIG_SLOPE = 1.702


def expert_grads(packed):
    x_rows, dy_rows, weight_rows, gate_w, up_w, down_w = packed
    gate_pre = jnp.dot(x_rows, gate_w, preferred_element_type=jnp.float32)
    up_pre = jnp.dot(x_rows, up_w, preferred_element_type=jnp.float32)
    gate_clamp = jnp.minimum(gate_pre, CLAMP_LIMIT)
    up_clamp = jnp.clip(up_pre, -CLAMP_LIMIT, CLAMP_LIMIT)
    sig = jax.nn.sigmoid(SIG_SLOPE * gate_clamp)
    act = (gate_clamp * sig * (up_clamp + 1.0)).astype(jnp.bfloat16)
    back = lax.dot_general(dy_rows, down_w, (((1,), (1,)), ((), ())), preferred_element_type=jnp.float32)
    weight_grad = jnp.sum(act.astype(jnp.float32) * back, axis=1).astype(jnp.bfloat16)
    route_col = weight_rows.astype(jnp.float32)[:, None]
    d_act = route_col * back
    d_gate = jnp.where(gate_pre < CLAMP_LIMIT, d_act * (up_clamp + 1.0) * (sig + SIG_SLOPE * gate_clamp * sig * (1.0 - sig)), 0.0).astype(jnp.bfloat16)
    d_up = jnp.where(jnp.abs(up_pre) < CLAMP_LIMIT, d_act * gate_clamp * sig, 0.0).astype(jnp.bfloat16)
    scaled_cot = (route_col * dy_rows.astype(jnp.float32)).astype(jnp.bfloat16)
    contract_rows = (((0,), (0,)), ((), ()))
    grad_gate = lax.dot_general(x_rows, d_gate, contract_rows, preferred_element_type=jnp.float32)
    grad_up = lax.dot_general(x_rows, d_up, contract_rows, preferred_element_type=jnp.float32)
    grad_down = lax.dot_general(act, scaled_cot, contract_rows, preferred_element_type=jnp.float32)
    slot_count, hidden = d_gate.shape
    model_width = gate_w.shape[0]
    group = hidden // N_TP
    partials = jnp.einsum('sjf,djf->jsd', d_gate.astype(jnp.float32).reshape(slot_count, N_TP, group), gate_w.astype(jnp.float32).reshape(model_width, N_TP, group))
    partials = partials + jnp.einsum('sjf,djf->jsd', d_up.astype(jnp.float32).reshape(slot_count, N_TP, group), up_w.astype(jnp.float32).reshape(model_width, N_TP, group))
    rounded = lax.optimization_barrier(partials.astype(jnp.bfloat16))
    row_grad = jnp.sum(rounded.astype(jnp.float32), axis=0).astype(jnp.bfloat16)
    return grad_gate, grad_up, grad_down, row_grad, weight_grad


def reference(tokens, cotangent, route_ids, route_weights, w_gate, w_up, w_down, dense_in, dense_out, dense_gate):
    total_tokens, model_width = tokens.shape
    top_k = route_ids.shape[1]
    expert_count = w_gate.shape[0]
    per_device = total_tokens // N_EP
    ids = route_ids.reshape(N_EP, per_device * top_k).astype(jnp.int32)
    one_hot = (ids[:, :, None] == jnp.arange(expert_count, dtype=jnp.int32)[None, None, :]).astype(jnp.int32)
    earlier = jnp.cumsum(one_hot, axis=1) - one_hot
    slot_index = jnp.sum(earlier * one_hot, axis=2)
    source_dev = jnp.arange(N_EP, dtype=jnp.int32)[:, None]
    position = (ids * (N_EP * CAP) + source_dev * CAP + slot_index).reshape(-1).astype(jnp.int32)
    token_of = (jnp.arange(total_tokens * top_k, dtype=jnp.int32) // top_k).astype(jnp.int32)
    slot_total = expert_count * N_EP * CAP
    x_buf = jnp.zeros((slot_total, model_width), jnp.bfloat16).at[position].set(tokens[token_of]).reshape(expert_count, N_EP * CAP, model_width)
    dy_buf = jnp.zeros((slot_total, model_width), jnp.bfloat16).at[position].set(cotangent[token_of]).reshape(expert_count, N_EP * CAP, model_width)
    weight_buf = jnp.zeros((slot_total,), jnp.bfloat16).at[position].set(route_weights.reshape(-1)).reshape(expert_count, N_EP * CAP)
    grad_gate, grad_up, grad_down, row_grad, weight_grad = lax.map(expert_grads, (x_buf, dy_buf, weight_buf, w_gate, w_up, w_down))
    expert_dx = row_grad.reshape(slot_total, model_width)[position].astype(jnp.float32).reshape(total_tokens, top_k, model_width)
    expert_dx = jnp.sum(expert_dx, axis=1)
    grad_route_weights = weight_grad.reshape(-1)[position].reshape(total_tokens, top_k)

    dense_pre = jnp.dot(tokens, dense_in, preferred_element_type=jnp.float32)
    dense_act = jax.nn.silu(dense_pre).astype(jnp.bfloat16)
    dense_val = lax.dot_general(dense_act, dense_out, (((1,), (1,)), ((), ())), preferred_element_type=jnp.float32)
    mix = jax.nn.sigmoid(jnp.dot(tokens, dense_gate, preferred_element_type=jnp.float32))
    cot_wide = cotangent.astype(jnp.float32)
    dense_scaled = (mix[:, None] * cot_wide).astype(jnp.bfloat16)
    dense_back = jnp.dot(dense_scaled, dense_out, preferred_element_type=jnp.float32)
    sig_pre = jax.nn.sigmoid(dense_pre)
    dense_dpre = (dense_back * sig_pre * (1.0 + dense_pre * (1.0 - sig_pre))).astype(jnp.bfloat16)
    dlogit = mix * (1.0 - mix) * jnp.sum(cot_wide * dense_val, axis=1)
    dense_dx = lax.dot_general(dense_dpre, dense_in, (((1,), (1,)), ((), ())), preferred_element_type=jnp.float32)
    dense_dx = dense_dx + dlogit[:, None] * dense_gate.astype(jnp.float32)[None, :]
    grad_tokens = (dense_dx + expert_dx).astype(jnp.bfloat16)
    contract_rows = (((0,), (0,)), ((), ()))
    grad_dense_in = lax.dot_general(tokens, dense_dpre, contract_rows, preferred_element_type=jnp.float32)
    grad_dense_out = lax.dot_general(dense_scaled, dense_act, contract_rows, preferred_element_type=jnp.float32)
    grad_dense_gate = jnp.sum(tokens.astype(jnp.float32) * dlogit[:, None], axis=0)
    return (grad_tokens, grad_route_weights, grad_gate, grad_up, grad_down, grad_dense_in, grad_dense_out, grad_dense_gate)
```

```python
import jax
import jax.numpy as jnp
from jax import lax
from jax.sharding import PartitionSpec as P

CLAMP_LIMIT = 7.0
SIG_SLOPE = 1.702
F32 = jnp.float32
BF16 = jnp.bfloat16
COLS = (((1,), (1,)), ((), ()))
ROWS = (((0,), (0,)), ((), ()))


def mm(a, b, dims=(((1,), (0,)), ((), ()))):
    return lax.dot_general(a, b, dims, preferred_element_type=F32)


def shards(
    tokens,
    cotangent,
    route_ids,
    route_weights,
    w_gate,
    w_up,
    w_down,
    dense_in,
    dense_out,
    dense_gate,
):
    n_ep = lax.axis_size("ep")
    n_tp = lax.axis_size("tp")
    tp = lax.axis_index("tp")
    tok, width = tokens.shape
    top = route_ids.shape[1]
    cap = 2 * tok * top // n_ep
    slots = n_ep * cap
    quarter = width // n_tp
    up = [(k, (k + 1) % n_tp) for k in range(n_tp)]
    down = [(k, (k - 1) % n_tp) for k in range(n_tp)]
    own, nxt, prv, far = tp, (tp + 1) % n_tp, (tp + 3) % n_tp, (tp + 2) % n_tp

    def cols(a, q):
        return lax.dynamic_slice_in_dim(a, q * quarter, quarter, 1)

    def rows(a, q):
        return lax.dynamic_slice_in_dim(a, q * quarter, quarter, 0)

    def exchange(a):
        return lax.all_to_all(a, "ep", split_axis=0, concat_axis=0, tiled=True)

    ids = route_ids.T
    wts = route_weights.T
    experts = lax.broadcasted_iota(jnp.int32, (n_ep, tok), 0)
    picks = [ids[k][None, :] == experts for k in range(top)]
    named = picks[0] | picks[1]
    earlier = (
        lax.broadcasted_iota(jnp.int32, (tok, tok), 0)
        < lax.broadcasted_iota(jnp.int32, (tok, tok), 1)
    ).astype(BF16)
    rank = mm(named.astype(BF16), earlier).astype(jnp.int32)
    key = jnp.where(named, rank, -1)
    hit = key[:, None, :] == lax.broadcasted_iota(jnp.int32, (n_ep, cap, tok), 1)
    place = hit.astype(BF16).reshape(slots, tok)
    share = jnp.where(picks[0], wts[0][None, :], 0) + jnp.where(picks[1], wts[1][None, :], 0)
    place_w = jnp.where(hit, share.astype(BF16)[:, None, :], 0).astype(BF16).reshape(slots, tok)

    def pair(a):
        return jnp.concatenate([cols(a, own), cols(a, nxt)], axis=1)

    x_send = mm(place, pair(tokens)).astype(BF16).reshape(n_ep, cap, 2 * quarter)
    y_send = mm(place_w, pair(cotangent)).astype(BF16).reshape(n_ep, cap, 2 * quarter)
    x_got = exchange(x_send).reshape(slots, 2 * quarter)
    y_got = exchange(y_send).reshape(slots, 2 * quarter)

    def whole(got):
        a, b = got[:, :quarter], got[:, quarter:]
        c = lax.ppermute(a, "tp", up)
        d = lax.ppermute(b, "tp", down)
        full = jnp.zeros((slots, width), BF16)
        for piece, q in ((a, own), (b, nxt), (c, prv), (d, far)):
            full = lax.dynamic_update_slice_in_dim(full, piece, q * quarter, 1)
        return full

    x_slots = whole(x_got)
    y_slots = whole(y_got)
    gate_w, up_w, down_w = w_gate[0], w_up[0], w_down[0]
    gate_pre = mm(x_slots, gate_w)
    up_pre = mm(x_slots, up_w)
    gate_clamp = jnp.minimum(gate_pre, CLAMP_LIMIT)
    up_clamp = jnp.clip(up_pre, -CLAMP_LIMIT, CLAMP_LIMIT)
    sig = jax.nn.sigmoid(SIG_SLOPE * gate_clamp)
    glu = gate_clamp * sig
    act = (glu * (up_clamp + 1.0)).astype(BF16)
    to_gate = jnp.where(
        gate_pre < CLAMP_LIMIT,
        (up_clamp + 1.0) * (sig + SIG_SLOPE * gate_clamp * sig * (1.0 - sig)),
        0.0,
    )
    to_up = jnp.where(jnp.abs(up_pre) < CLAMP_LIMIT, glu, 0.0)
    back = mm(y_slots, down_w, COLS)
    d_gate = (back * to_gate).astype(BF16)
    d_up = (back * to_up).astype(BF16)
    w_part = jnp.sum(act.astype(F32) * back, axis=1)

    def partial(q):
        return mm(d_gate, rows(gate_w, q), COLS) + mm(d_up, rows(up_w, q), COLS)

    sent_prv = lax.ppermute(partial(prv).astype(BF16), "tp", down)
    sent_far = lax.ppermute(partial(far).astype(BF16), "tp", up)
    keep_own = (partial(own) + sent_prv.astype(F32)).astype(BF16)
    keep_nxt = (partial(nxt) + sent_far.astype(F32)).astype(BF16)
    back_rows = exchange(
        jnp.concatenate([keep_own, keep_nxt], axis=1).reshape(n_ep, cap, 2 * quarter)
    ).reshape(slots, 2 * quarter)

    w_back = exchange(w_part.reshape(n_ep, 1, cap)).reshape(n_ep, cap)
    w_back = w_back + lax.ppermute(w_back, "tp", [(k, k ^ 1) for k in range(n_tp)])
    w_back = w_back + lax.ppermute(w_back, "tp", [(k, k ^ 2) for k in range(n_tp)])
    per_expert = jnp.sum(jnp.where(hit, w_back[:, :, None], 0.0), axis=1)
    grad_route_weights = jnp.stack(
        [
            jnp.sum(jnp.where(picks[k], per_expert, 0.0), axis=0) / wts[k].astype(F32)
            for k in range(top)
        ],
        axis=1,
    ).astype(BF16)

    grad_gate = mm(x_slots, d_gate, ROWS)
    grad_up = mm(x_slots, d_up, ROWS)
    grad_down = mm(act, y_slots, ROWS)

    both = lax.all_gather(
        jnp.concatenate([dense_in, dense_out], axis=1), ("ep", "tp"), axis=0, tiled=True
    )
    hidden = dense_in.shape[1]
    in_whole, out_whole = both[:, :hidden], both[:, hidden:]
    dense_pre = mm(tokens, in_whole)
    dense_act = jax.nn.silu(dense_pre).astype(BF16)
    dense_val = mm(dense_act, out_whole, COLS)
    mix = jax.nn.sigmoid(jnp.dot(tokens, dense_gate, preferred_element_type=F32))
    cot_wide = cotangent.astype(F32)
    dense_scaled = (mix[:, None] * cot_wide).astype(BF16)
    dense_back = mm(dense_scaled, out_whole)
    sig_pre = jax.nn.sigmoid(dense_pre)
    dense_dpre = (dense_back * sig_pre * (1.0 + dense_pre * (1.0 - sig_pre))).astype(BF16)
    dlogit = mix * (1.0 - mix) * jnp.sum(cot_wide * dense_val, axis=1)
    dense_dx = mm(dense_dpre, rows(in_whole, own), COLS)
    gate_cols = lax.dynamic_slice_in_dim(dense_gate, own * quarter, quarter, 0)
    dense_dx = dense_dx + dlogit[:, None] * gate_cols.astype(F32)[None, :]

    block = width // (n_ep * n_tp)

    def mine(a):
        return lax.dynamic_index_in_dim(
            a.reshape(tok, n_ep, n_tp, block), own, 2, keepdims=False
        ).reshape(tok, n_ep * block)

    tokens_own = mine(tokens)
    in_part = mm(tokens_own, dense_dpre, ROWS)
    out_part = mm(mine(dense_scaled), dense_act, ROWS)
    gate_part = jnp.sum(tokens_own.astype(F32) * dlogit[:, None], axis=0)
    summed = lax.psum_scatter(
        jnp.concatenate([in_part, out_part, gate_part[:, None]], axis=1),
        "ep",
        scatter_dimension=0,
        tiled=True,
    )

    got = mm(place, back_rows, ROWS)
    others = lax.ppermute(got[:, quarter:].astype(BF16), "tp", up)
    grad_tokens = (dense_dx + got[:, :quarter] + others.astype(F32)).astype(BF16)
    return (
        grad_tokens,
        grad_route_weights,
        grad_gate[None],
        grad_up[None],
        grad_down[None],
        summed[:, :hidden],
        summed[:, hidden : 2 * hidden],
        summed[:, 2 * hidden],
    )


def solution(mesh):
    both = ("ep", "tp")
    return jax.shard_map(
        shards,
        mesh=mesh,
        in_specs=(
            P("ep", None),
            P("ep", None),
            P("ep", None),
            P("ep", None),
            P("ep", None, "tp"),
            P("ep", None, "tp"),
            P("ep", "tp", None),
            P(both, None),
            P(both, None),
            P(),
        ),
        out_specs=(
            P("ep", "tp"),
            P("ep", None),
            P("ep", None, "tp"),
            P("ep", None, "tp"),
            P("ep", "tp", None),
            P(both, None),
            P(both, None),
            P(both),
        ),
        check_vma=False,
    )
```

```python
import jax
import jax.numpy as jnp
from jax import lax
from jax.sharding import PartitionSpec as P


CLAMP_LIMIT = 7.0
SIG_SLOPE = 1.702
F32 = jnp.float32
BF16 = jnp.bfloat16
COLS = (((1,), (1,)), ((), ()))
ROWS = (((0,), (0,)), ((), ()))


def mm(a, b, dims=(((1,), (0,)), ((), ()))):
    return lax.dot_general(a, b, dims, preferred_element_type=F32)


def shards(
    tokens,
    cotangent,
    route_ids,
    route_weights,
    w_gate,
    w_up,
    w_down,
    dense_in,
    dense_out,
    dense_gate,
):
    n_ep = lax.axis_size("ep")
    n_tp = lax.axis_size("tp")
    tp = lax.axis_index("tp")
    tok, width = tokens.shape
    top = route_ids.shape[1]
    cap = 2 * tok * top // n_ep
    slots = n_ep * cap
    quarter = width // n_tp
    up = [(k, (k + 1) % n_tp) for k in range(n_tp)]
    down = [(k, (k - 1) % n_tp) for k in range(n_tp)]
    own, nxt, prv, far = tp, (tp + 1) % n_tp, (tp + 3) % n_tp, (tp + 2) % n_tp

    def cols(a, q):
        return lax.dynamic_slice_in_dim(a, q * quarter, quarter, 1)

    def rows(a, q):
        return lax.dynamic_slice_in_dim(a, q * quarter, quarter, 0)

    def exchange(a):
        return lax.all_to_all(a, "ep", split_axis=0, concat_axis=0, tiled=True)

    ids = route_ids.T
    wts = route_weights.T
    experts = lax.broadcasted_iota(jnp.int32, (n_ep, tok), 0)
    picks = [ids[k][None, :] == experts for k in range(top)]
    named = picks[0] | picks[1]
    earlier = (
        lax.broadcasted_iota(jnp.int32, (tok, tok), 0)
        < lax.broadcasted_iota(jnp.int32, (tok, tok), 1)
    ).astype(BF16)
    rank = mm(named.astype(BF16), earlier).astype(jnp.int32)
    key = jnp.where(named, rank, -1)
    hit = key[:, None, :] == lax.broadcasted_iota(jnp.int32, (n_ep, cap, tok), 1)
    place = hit.astype(BF16).reshape(slots, tok)
    share = jnp.where(picks[0], wts[0][None, :], 0) + jnp.where(picks[1], wts[1][None, :], 0)
    place_w = jnp.where(hit, share.astype(BF16)[:, None, :], 0).astype(BF16).reshape(slots, tok)

    x_send = mm(place, cols(tokens, own)).astype(BF16).reshape(n_ep, cap, quarter)
    y_pair = jnp.concatenate([cols(cotangent, own), cols(cotangent, nxt)], axis=1)
    y_send = mm(place_w, y_pair).astype(BF16).reshape(n_ep, cap, 2 * quarter)
    x_got = exchange(x_send).reshape(slots, quarter)
    y_got = exchange(y_send).reshape(slots, 2 * quarter)

    def put(full, piece, q):
        return lax.dynamic_update_slice_in_dim(full, piece, q * quarter, 1)

    half = slots // 2
    x_up = lax.ppermute(x_got, "tp", up)
    x_dn = lax.ppermute(x_got, "tp", down)
    x_far_a = lax.ppermute(x_dn[:half], "tp", down)
    x_far_b = lax.ppermute(x_up[half:], "tp", up)
    x_slots = jnp.zeros((slots, width), BF16)
    for piece, q in ((x_got, own), (x_up, prv), (x_dn, nxt)):
        x_slots = put(x_slots, piece, q)
    x_slots = lax.dynamic_update_slice(x_slots, x_far_a, (0, far * quarter))
    x_slots = lax.dynamic_update_slice(x_slots, x_far_b, (half, far * quarter))
    y_a, y_b = y_got[:, :quarter], y_got[:, quarter:]
    y_up = lax.ppermute(y_a, "tp", up)
    y_dn = lax.ppermute(y_b, "tp", down)
    y_slots = jnp.zeros((slots, width), BF16)
    for piece, q in ((y_a, own), (y_b, nxt), (y_up, prv), (y_dn, far)):
        y_slots = put(y_slots, piece, q)

    gate_w, up_w, down_w = w_gate[0], w_up[0], w_down[0]
    gate_pre = mm(x_slots, gate_w)
    up_pre = mm(x_slots, up_w)
    gate_clamp = jnp.minimum(gate_pre, CLAMP_LIMIT)
    up_clamp = jnp.clip(up_pre, -CLAMP_LIMIT, CLAMP_LIMIT)
    sig = jax.nn.sigmoid(SIG_SLOPE * gate_clamp)
    glu = gate_clamp * sig
    act = (glu * (up_clamp + 1.0)).astype(BF16)
    to_gate = jnp.where(
        gate_pre < CLAMP_LIMIT,
        (up_clamp + 1.0) * (sig + SIG_SLOPE * gate_clamp * sig * (1.0 - sig)),
        0.0,
    )
    to_up = jnp.where(jnp.abs(up_pre) < CLAMP_LIMIT, glu, 0.0)
    act, to_gate, to_up = lax.optimization_barrier((act, to_gate, to_up))
    tokens, cotangent, act = lax.optimization_barrier((tokens, cotangent, act))
    back = mm(y_slots, down_w, COLS)
    d_gate = (back * to_gate).astype(BF16)
    d_up = (back * to_up).astype(BF16)
    w_part = jnp.sum(act.astype(F32) * back, axis=1)

    def partial(q):
        return mm(d_gate, rows(gate_w, q), COLS) + mm(d_up, rows(up_w, q), COLS)

    away = partial(far).astype(BF16)
    top_in = lax.ppermute(away[:half], "tp", up)
    low_in = lax.ppermute(away[half:], "tp", down)
    ahead = partial(nxt)
    ahead = jnp.concatenate([ahead[:half] + top_in.astype(F32), ahead[half:]], axis=0).astype(BF16)
    behind = partial(prv)
    behind = jnp.concatenate([behind[:half], behind[half:] + low_in.astype(F32)], axis=0)
    behind = behind.astype(BF16)
    ahead = lax.ppermute(ahead, "tp", up)
    behind = lax.ppermute(behind, "tp", down)
    total = partial(own) + ahead.astype(F32) + behind.astype(F32)
    back_rows = exchange(total.astype(BF16).reshape(n_ep, cap, quarter))
    back_rows = back_rows.reshape(slots, quarter)

    w_back = exchange(w_part.reshape(n_ep, 1, cap)).reshape(n_ep, cap)
    w_back = w_back + lax.ppermute(w_back, "tp", [(k, k ^ 1) for k in range(n_tp)])
    w_back = w_back + lax.ppermute(w_back, "tp", [(k, k ^ 2) for k in range(n_tp)])
    per_expert = jnp.sum(jnp.where(hit, w_back[:, :, None], 0.0), axis=1)
    grad_route_weights = jnp.stack(
        [
            jnp.sum(jnp.where(picks[k], per_expert, 0.0), axis=0) / wts[k].astype(F32)
            for k in range(top)
        ],
        axis=1,
    ).astype(BF16)

    grad_gate = mm(x_slots, d_gate, ROWS)
    grad_up = mm(x_slots, d_up, ROWS)
    grad_down = mm(act, y_slots, ROWS)

    both = lax.all_gather(
        jnp.concatenate([dense_in, dense_out], axis=1), ("ep", "tp"), axis=0, tiled=True
    )
    hidden = dense_in.shape[1]
    in_whole, out_whole = both[:, :hidden], both[:, hidden:]
    dense_pre = mm(tokens, in_whole)
    dense_act = jax.nn.silu(dense_pre).astype(BF16)
    cot_out = mm(cotangent, out_whole)
    mix = jax.nn.sigmoid(jnp.dot(tokens, dense_gate, preferred_element_type=F32))
    dense_scaled = (mix[:, None] * cotangent.astype(F32)).astype(BF16)
    dense_back = mm(dense_scaled, out_whole)
    sig_pre = jax.nn.sigmoid(dense_pre)
    dense_dpre = (dense_back * sig_pre * (1.0 + dense_pre * (1.0 - sig_pre))).astype(BF16)
    dlogit = mix * (1.0 - mix) * jnp.sum(dense_act.astype(F32) * cot_out, axis=1)
    dense_dx = mm(dense_dpre, rows(in_whole, own), COLS)
    gate_cols = lax.dynamic_slice_in_dim(dense_gate, own * quarter, quarter, 0)
    dense_dx = dense_dx + dlogit[:, None] * gate_cols.astype(F32)[None, :]

    block = width // (n_ep * n_tp)

    def mine(a):
        return lax.dynamic_index_in_dim(
            a.reshape(tok, n_ep, n_tp, block), own, 2, keepdims=False
        ).reshape(tok, n_ep * block)

    tokens_own = mine(tokens)
    in_part = mm(tokens_own, dense_dpre, ROWS)
    out_part = mm(mine(dense_scaled), dense_act, ROWS)
    gate_part = jnp.sum(tokens_own.astype(F32) * dlogit[:, None], axis=0)
    summed = lax.psum_scatter(
        jnp.concatenate([in_part, out_part, gate_part[:, None]], axis=1),
        "ep",
        scatter_dimension=0,
        tiled=True,
    )

    grad_tokens = (dense_dx + mm(place, back_rows, ROWS)).astype(BF16)
    return (
        grad_tokens,
        grad_route_weights,
        grad_gate[None],
        grad_up[None],
        grad_down[None],
        summed[:, :hidden],
        summed[:, hidden : 2 * hidden],
        summed[:, 2 * hidden],
    )


def solution(mesh):
    both = ("ep", "tp")

    return jax.shard_map(
        shards,
        mesh=mesh,
        in_specs=(
            P("ep", None),
            P("ep", None),
            P("ep", None),
            P("ep", None),
            P("ep", None, "tp"),
            P("ep", None, "tp"),
            P("ep", "tp", None),
            P(both, None),
            P(both, None),
            P(),
        ),
        out_specs=(
            P("ep", "tp"),
            P("ep", None),
            P("ep", None, "tp"),
            P("ep", None, "tp"),
            P("ep", "tp", None),
            P(both, None),
            P(both, None),
            P(both),
        ),
        check_vma=False,
    )
```

```python
import jax
import jax.numpy as jnp
from jax import lax
from jax.experimental import pallas as pl
from jax.experimental.pallas import tpu as pltpu
from jax.sharding import PartitionSpec as P


CLAMP_LIMIT = 7.0
SIG_SLOPE = 1.702
F32 = jnp.float32
BF16 = jnp.bfloat16
PLAIN = (((1,), (0,)), ((), ()))
COLS = (((1,), (1,)), ((), ()))
ROWS = (((0,), (0,)), ((), ()))
TILES = 4


def mm(a, b, dims=PLAIN):
    return lax.dot_general(a, b, dims, preferred_element_type=F32)


def call(body, grid, q, ins, outs, flops):
    nbytes = sum(a.size * a.dtype.itemsize for a, _ in ins)
    nbytes += sum(a.size * a.dtype.itemsize for a, _ in outs)
    return pl.pallas_call(
        body,
        grid_spec=pltpu.PrefetchScalarGridSpec(
            num_scalar_prefetch=1,
            grid=(grid,),
            in_specs=[spec for _, spec in ins],
            out_specs=[spec for _, spec in outs],
        ),
        out_shape=[a for a, _ in outs],
        cost_estimate=pl.CostEstimate(flops=flops, bytes_accessed=nbytes, transcendentals=0),
    )(q, *[a for a, _ in ins])


def first_parts(q, xa, xn, xp, ya, yb, ga, gn, gp, ua, un, up, da, dn, gate_o, up_o, back_o):
    gate_o[...] = mm(xa[...], ga[...]) + mm(xn[...], gn[...]) + mm(xp[...], gp[...])
    up_o[...] = mm(xa[...], ua[...]) + mm(xn[...], un[...]) + mm(xp[...], up[...])
    back_o[...] = mm(ya[...], da[...]) + mm(yb[...], dn[...])


def last_parts(
    q, gate_in, up_in, back_in, xf, yp, yf, gf, uf, dp, df, gt, ut, act_o, dgate_o, dup_o, w_o, away_o
):
    gate_pre = gate_in[...] + mm(xf[...], gf[...])
    up_pre = up_in[...] + mm(xf[...], uf[...])
    gate_clamp = jnp.minimum(gate_pre, CLAMP_LIMIT)
    up_clamp = jnp.clip(up_pre, -CLAMP_LIMIT, CLAMP_LIMIT)
    sig = jax.nn.sigmoid(SIG_SLOPE * gate_clamp)
    glu = gate_clamp * sig
    act = (glu * (up_clamp + 1.0)).astype(BF16)
    act_o[...] = act
    back = back_in[...] + mm(yp[...], dp[...]) + mm(yf[...], df[...])
    w_o[...] = jnp.sum(act.astype(F32) * back, axis=1, keepdims=True)
    slope = (up_clamp + 1.0) * (sig + SIG_SLOPE * gate_clamp * sig * (1.0 - sig))
    d_gate = jnp.where(gate_pre < CLAMP_LIMIT, back * slope, 0.0).astype(BF16)
    d_up = jnp.where(jnp.abs(up_pre) < CLAMP_LIMIT, back * glu, 0.0).astype(BF16)
    dgate_o[...] = d_gate
    dup_o[...] = d_up
    away_o[...] = (mm(d_gate, gt[...]) + mm(d_up, ut[...])).astype(BF16)


def next_parts(q, dg, du, gn, un, gp, up, top, low, ahead_o, behind_o):
    first = pl.program_id(0) < TILES // 2
    ahead = mm(dg[...], gn[...]) + mm(du[...], un[...])
    behind = mm(dg[...], gp[...]) + mm(du[...], up[...])
    ahead_o[...] = (ahead + jnp.where(first, top[...].astype(F32), 0.0)).astype(BF16)
    behind_o[...] = (behind + jnp.where(first, 0.0, low[...].astype(F32))).astype(BF16)


def own_part(q, dg, du, ga, ua, out):
    out[...] = (mm(dg[...], ga[...]) + mm(du[...], ua[...])).astype(BF16)


def weight_grads(q, xa, xn, xp, xf, ya, yn, yp, yf, dg, du, act, gate_o, up_o, down_o):
    for k, (x, y) in enumerate(((xa, ya), (xn, yn), (xp, yp), (xf, yf))):

        @pl.when(pl.program_id(0) == k)
        def _():
            gate_o[...] = mm(x[...], dg[...], ROWS)
            up_o[...] = mm(x[...], du[...], ROWS)
            down_o[...] = mm(act[...], y[...], ROWS)


def shards(
    tokens,
    cotangent,
    route_ids,
    route_weights,
    w_gate,
    w_up,
    w_down,
    dense_in,
    dense_out,
    dense_gate,
):
    n_ep = lax.axis_size("ep")
    n_tp = lax.axis_size("tp")
    tp = lax.axis_index("tp")
    tok, width = tokens.shape
    top = route_ids.shape[1]
    cap = 2 * tok * top // n_ep
    slots = n_ep * cap
    quarter = width // n_tp
    hid = w_gate.shape[2]
    thin, hidden = dense_in.shape
    up = [(k, (k + 1) % n_tp) for k in range(n_tp)]
    down = [(k, (k - 1) % n_tp) for k in range(n_tp)]
    own, nxt, prv, far = tp, (tp + 1) % n_tp, (tp + 3) % n_tp, (tp + 2) % n_tp
    q = jnp.stack([own, nxt, prv, far]).astype(jnp.int32)

    def cols(a, k):
        return lax.dynamic_slice_in_dim(a, k * quarter, quarter, 1)

    def exchange(a):
        return lax.all_to_all(a, "ep", split_axis=0, concat_axis=0, tiled=True)

    ids = route_ids.T
    wts = route_weights.T
    experts = lax.broadcasted_iota(jnp.int32, (n_ep, tok), 0)
    picks = [ids[k][None, :] == experts for k in range(top)]
    named = picks[0] | picks[1]
    earlier = (
        lax.broadcasted_iota(jnp.int32, (tok, tok), 0)
        < lax.broadcasted_iota(jnp.int32, (tok, tok), 1)
    ).astype(BF16)
    rank = mm(named.astype(BF16), earlier).astype(jnp.int32)
    key = jnp.where(named, rank, -1)
    hit = key[:, None, :] == lax.broadcasted_iota(jnp.int32, (n_ep, cap, tok), 1)
    place = hit.astype(BF16).reshape(slots, tok)
    share = jnp.where(picks[0], wts[0][None, :], 0) + jnp.where(picks[1], wts[1][None, :], 0)
    place_w = jnp.where(hit, share.astype(BF16)[:, None, :], 0).astype(BF16).reshape(slots, tok)

    full = cap + thin
    key_more = jnp.concatenate(
        [key, lax.broadcasted_iota(jnp.int32, (n_ep, thin), 1) + cap], axis=1
    )
    hit_more = key_more[:, None, :] == lax.broadcasted_iota(
        jnp.int32, (n_ep, full, tok + thin), 1
    )
    mine = jnp.concatenate([dense_in, dense_out], axis=1)
    rows = jnp.concatenate([cols(tokens, own), mine], axis=0)
    x_send = mm(hit_more.astype(BF16).reshape(n_ep * full, tok + thin), rows)
    x_send = x_send.astype(BF16).reshape(n_ep, full, quarter)
    x_all = exchange(x_send)
    gate_w, up_w, down_w = w_gate[0], w_up[0], w_down[0]
    x_all, gate_t, up_t, down_t = lax.optimization_barrier(
        (x_all, gate_w.T, up_w.T, down_w.T)
    )
    y_pair = jnp.concatenate([cols(cotangent, own), cols(cotangent, nxt)], axis=1)
    y_send = mm(place_w, y_pair).astype(BF16).reshape(n_ep, cap, 2 * quarter)
    f_send = mm(place, cols(tokens, far)).astype(BF16).reshape(n_ep, cap, quarter)

    def owned(a):
        return lax.dynamic_index_in_dim(
            a.reshape(tok, n_ep, n_tp, thin), own, 2, keepdims=False
        ).reshape(tok, n_ep * thin)

    tokens_own, cot_own = owned(tokens), owned(cotangent)
    f_send, tokens_own, cot_own = lax.optimization_barrier((f_send, tokens_own, cot_own))
    y_got = exchange(y_send).reshape(slots, 2 * quarter)
    x_far = exchange(f_send).reshape(slots, quarter)
    x_all_up = lax.ppermute(x_all, "tp", up)
    x_all_dn = lax.ppermute(x_all, "tp", down)
    x_own = x_all[:, :cap].reshape(slots, quarter)
    x_prv, x_nxt = [a[:, :cap].reshape(slots, quarter) for a in (x_all_up, x_all_dn)]
    d_own, d_prv, d_nxt = [a[:, cap:] for a in (x_all, x_all_up, x_all_dn)]
    d_far_low = lax.ppermute(d_prv[n_ep // 2 :], "tp", up)
    d_far_top = lax.ppermute(d_nxt[: n_ep // 2], "tp", down)
    y_own, y_nxt = y_got[:, :quarter], y_got[:, quarter:]
    y_prv = lax.ppermute(y_own, "tp", up)
    y_far = lax.ppermute(y_nxt, "tp", down)

    tile = slots // TILES

    def by_tile(a):
        return a, pl.BlockSpec((tile, a.shape[1]), lambda t, q: (t, 0))

    def by_row(a, k):
        return a, pl.BlockSpec((quarter, hid), lambda t, q: (q[k], 0))

    def by_col(a, k):
        return a, pl.BlockSpec((hid, quarter), lambda t, q: (0, q[k]))

    def whole(a):
        return a, pl.BlockSpec(a.shape, lambda t, q: (0, 0))

    def wide(width_, dtype):
        return by_tile(jax.ShapeDtypeStruct((slots, width_), dtype))

    unit = 2 * slots * quarter * hid
    parts = call(
        first_parts,
        TILES,
        q,
        [by_tile(a) for a in (x_own, x_nxt, x_prv, y_own, y_nxt)]
        + [by_row(gate_w, k) for k in range(3)]
        + [by_row(up_w, k) for k in range(3)]
        + [by_row(down_t, k) for k in range(2)],
        [wide(hid, F32)] * 3,
        8 * unit,
    )
    act, d_gate, d_up, w_part, away = call(
        last_parts,
        TILES,
        q,
        [by_tile(a) for a in (*parts, x_far, y_prv, y_far)]
        + [by_row(gate_w, 3), by_row(up_w, 3), by_row(down_t, 2), by_row(down_t, 3)]
        + [by_col(gate_t, 3), by_col(up_t, 3)],
        [wide(hid, BF16)] * 3 + [wide(1, F32), wide(quarter, BF16)],
        6 * unit,
    )
    half = slots // 2
    top_in = lax.ppermute(away[:half], "tp", up)
    low_in = lax.ppermute(away[half:], "tp", down)
    ahead, behind = call(
        next_parts,
        TILES,
        q,
        [by_tile(d_gate), by_tile(d_up), by_col(gate_t, 1), by_col(up_t, 1)]
        + [by_col(gate_t, 2), by_col(up_t, 2)]
        + [
            (top_in, pl.BlockSpec((tile, quarter), lambda t, q: (lax.min(t, TILES // 2 - 1), 0))),
            (low_in, pl.BlockSpec((tile, quarter), lambda t, q: (lax.max(t - TILES // 2, 0), 0))),
        ],
        [wide(quarter, BF16)] * 2,
        4 * unit,
    )
    ahead = lax.ppermute(ahead, "tp", up)
    behind = lax.ppermute(behind, "tp", down)
    (mid,) = call(
        own_part,
        TILES,
        q,
        [by_tile(d_gate), by_tile(d_up), by_col(gate_t, 0), by_col(up_t, 0)],
        [wide(quarter, BF16)],
        2 * unit,
    )
    total = (mid.astype(F32) + ahead.astype(F32) + behind.astype(F32)).astype(BF16)
    back_rows = exchange(total.reshape(n_ep, cap, quarter)).reshape(slots, quarter)

    grad_gate, grad_up, grad_down = call(
        weight_grads,
        n_tp,
        q,
        [whole(a) for a in (x_own, x_nxt, x_prv, x_far, y_own, y_nxt, y_prv, y_far)]
        + [whole(d_gate), whole(d_up), whole(act)],
        [
            (jax.ShapeDtypeStruct((width, hid), F32), pl.BlockSpec((quarter, hid), lambda t, q: (q[t], 0))),
            (jax.ShapeDtypeStruct((width, hid), F32), pl.BlockSpec((quarter, hid), lambda t, q: (q[t], 0))),
            (jax.ShapeDtypeStruct((hid, width), F32), pl.BlockSpec((hid, quarter), lambda t, q: (0, q[t]))),
        ],
        12 * unit,
    )

    d_far = jnp.concatenate([d_far_top, d_far_low], axis=0)
    both = jnp.zeros((n_ep, n_tp, thin, 2 * hidden), BF16)
    for piece, k in ((d_own, own), (d_nxt, nxt), (d_prv, prv), (d_far, far)):
        both = lax.dynamic_update_index_in_dim(both, piece, k, 1)
    both = both.reshape(width, 2 * hidden)
    in_whole, out_whole = both[:, :hidden], both[:, hidden:]
    dense_pre = mm(tokens, in_whole)
    dense_act = jax.nn.silu(dense_pre).astype(BF16)
    mix = jax.nn.sigmoid(jnp.dot(tokens, dense_gate, preferred_element_type=F32))
    dense_scaled = (mix[:, None] * cotangent.astype(F32)).astype(BF16)
    cot_out = mm(cotangent, out_whole)
    dense_back = mm(dense_scaled, out_whole)
    sig_pre = jax.nn.sigmoid(dense_pre)
    dense_dpre = (dense_back * sig_pre * (1.0 + dense_pre * (1.0 - sig_pre))).astype(BF16)
    dlogit = mix * (1.0 - mix) * jnp.sum(dense_act.astype(F32) * cot_out, axis=1)
    in_rows = lax.dynamic_slice_in_dim(in_whole, own * quarter, quarter, 0)
    dense_dx = mm(dense_dpre, in_rows, COLS)
    gate_cols = lax.dynamic_slice_in_dim(dense_gate, own * quarter, quarter, 0)
    dense_dx = dense_dx + dlogit[:, None] * gate_cols.astype(F32)[None, :]

    in_part = mm(tokens_own, dense_dpre, ROWS)
    scaled_own = (mix[:, None] * cot_own.astype(F32)).astype(BF16)
    out_part = mm(scaled_own, dense_act, ROWS)
    gate_part = jnp.sum(tokens_own.astype(F32) * dlogit[:, None], axis=0)
    sent = jnp.concatenate([in_part, out_part], axis=1).reshape(n_ep, thin, 2 * hidden)
    w_rows = w_part.reshape(n_ep, 1, cap)
    w_high = w_rows.astype(BF16)
    w_low = (w_rows - w_high.astype(F32)).astype(BF16)

    def line(a):
        return jnp.pad(a.astype(BF16), ((0, 0), (0, 0), (0, 2 * hidden - a.shape[2])))

    tail = jnp.concatenate([line(gate_part.reshape(n_ep, 1, thin)), line(w_high), line(w_low)], axis=1)
    tail = jnp.pad(tail, ((0, 0), (0, 5), (0, 0)))
    sent = jnp.concatenate([sent.astype(BF16), tail], axis=1)
    came = exchange(sent)
    summed = jnp.sum(came[:, : thin + 1].astype(F32), axis=0)
    w_back = came[:, thin + 1, :cap].astype(F32) + came[:, thin + 2, :cap].astype(F32)
    w_back = w_back + lax.ppermute(w_back, "tp", [(k, k ^ 1) for k in range(n_tp)])
    w_back = w_back + lax.ppermute(w_back, "tp", [(k, k ^ 2) for k in range(n_tp)])
    per_expert = jnp.sum(jnp.where(hit, w_back[:, :, None], 0.0), axis=1)
    grad_route_weights = jnp.stack(
        [
            jnp.sum(jnp.where(picks[k], per_expert, 0.0), axis=0) / wts[k].astype(F32)
            for k in range(top)
        ],
        axis=1,
    ).astype(BF16)
    grad_tokens = (dense_dx + mm(place, back_rows, ROWS)).astype(BF16)
    return (
        grad_tokens,
        grad_route_weights,
        grad_gate[None],
        grad_up[None],
        grad_down[None],
        summed[:thin, :hidden],
        summed[:thin, hidden:],
        summed[thin, :thin],
    )


def solution(mesh):
    both = ("ep", "tp")

    return jax.shard_map(
        shards,
        mesh=mesh,
        in_specs=(
            P("ep", None),
            P("ep", None),
            P("ep", None),
            P("ep", None),
            P("ep", None, "tp"),
            P("ep", None, "tp"),
            P("ep", "tp", None),
            P(both, None),
            P(both, None),
            P(),
        ),
        out_specs=(
            P("ep", "tp"),
            P("ep", None),
            P("ep", None, "tp"),
            P("ep", None, "tp"),
            P("ep", "tp", None),
            P(both, None),
            P(both, None),
            P(both),
        ),
        check_vma=False,
    )
```

```python
import jax
import jax.numpy as jnp
from jax import lax
from jax.experimental import pallas as pl
from jax.experimental.pallas import tpu as pltpu
from jax.sharding import PartitionSpec as P


CLAMP_LIMIT = 7.0
SIG_SLOPE = 1.702
F32 = jnp.float32
BF16 = jnp.bfloat16
PLAIN = (((1,), (0,)), ((), ()))
COLS = (((1,), (1,)), ((), ()))
ROWS = (((0,), (0,)), ((), ()))
TILES = 4


def mm(a, b, dims=PLAIN):
    return lax.dot_general(a, b, dims, preferred_element_type=F32)


def call(body, grid, q, ins, outs, flops):
    nbytes = sum(a.size * a.dtype.itemsize for a, _ in ins)
    nbytes += sum(a.size * a.dtype.itemsize for a, _ in outs)
    return pl.pallas_call(
        body,
        grid_spec=pltpu.PrefetchScalarGridSpec(
            num_scalar_prefetch=1,
            grid=(grid,),
            in_specs=[spec for _, spec in ins],
            out_specs=[spec for _, spec in outs],
        ),
        out_shape=[a for a, _ in outs],
        cost_estimate=pl.CostEstimate(flops=flops, bytes_accessed=nbytes, transcendentals=0),
    )(q, *[a for a, _ in ins])


def first_parts(q, xa, xn, xp, ya, yb, ga, gn, gp, ua, un, up, da, dn, gate_o, up_o, back_o):
    gate_o[...] = mm(xa[...], ga[...]) + mm(xn[...], gn[...]) + mm(xp[...], gp[...])
    up_o[...] = mm(xa[...], ua[...]) + mm(xn[...], un[...]) + mm(xp[...], up[...])
    back_o[...] = mm(ya[...], da[...]) + mm(yb[...], dn[...])


def last_parts(
    q, gate_in, up_in, back_in, xf, yp, yf, gf, uf, dp, df, *more
):
    turned, (act_o, dgate_o, dup_o, w_o, *parts_o) = more[:8], more[8:]
    gate_pre = gate_in[...] + mm(xf[...], gf[...])
    up_pre = up_in[...] + mm(xf[...], uf[...])
    gate_clamp = jnp.minimum(gate_pre, CLAMP_LIMIT)
    up_clamp = jnp.clip(up_pre, -CLAMP_LIMIT, CLAMP_LIMIT)
    sig = jax.nn.sigmoid(SIG_SLOPE * gate_clamp)
    glu = gate_clamp * sig
    act = (glu * (up_clamp + 1.0)).astype(BF16)
    act_o[...] = act
    back = back_in[...] + mm(yp[...], dp[...]) + mm(yf[...], df[...])
    w_o[...] = jnp.sum(act.astype(F32) * back, axis=1, keepdims=True)
    slope = (up_clamp + 1.0) * (sig + SIG_SLOPE * gate_clamp * sig * (1.0 - sig))
    d_gate = jnp.where(gate_pre < CLAMP_LIMIT, back * slope, 0.0).astype(BF16)
    d_up = jnp.where(jnp.abs(up_pre) < CLAMP_LIMIT, back * glu, 0.0).astype(BF16)
    dgate_o[...] = d_gate
    dup_o[...] = d_up
    for k, out in enumerate(parts_o):
        out[...] = (mm(d_gate, turned[k][...]) + mm(d_up, turned[4 + k][...])).astype(BF16)


def weight_grads(q, xa, xn, xp, xf, ya, yn, yp, yf, dg, du, act, gate_o, up_o, down_o):
    for k, (x, y) in enumerate(((xa, ya), (xn, yn), (xp, yp), (xf, yf))):

        @pl.when(pl.program_id(0) == k)
        def _():
            gate_o[...] = mm(x[...], dg[...], ROWS)
            up_o[...] = mm(x[...], du[...], ROWS)
            down_o[...] = mm(act[...], y[...], ROWS)


def shards(
    tokens,
    cotangent,
    route_ids,
    route_weights,
    w_gate,
    w_up,
    w_down,
    dense_in,
    dense_out,
    dense_gate,
):
    n_ep = lax.axis_size("ep")
    n_tp = lax.axis_size("tp")
    tp = lax.axis_index("tp")
    tok, width = tokens.shape
    top = route_ids.shape[1]
    cap = 2 * tok * top // n_ep
    slots = n_ep * cap
    quarter = width // n_tp
    hid = w_gate.shape[2]
    thin, hidden = dense_in.shape
    up = [(k, (k + 1) % n_tp) for k in range(n_tp)]
    down = [(k, (k - 1) % n_tp) for k in range(n_tp)]
    own, nxt, prv, far = tp, (tp + 1) % n_tp, (tp + 3) % n_tp, (tp + 2) % n_tp
    q = jnp.stack([own, nxt, prv, far]).astype(jnp.int32)

    def cols(a, k):
        return lax.dynamic_slice_in_dim(a, k * quarter, quarter, 1)

    def exchange(a):
        return lax.all_to_all(a, "ep", split_axis=0, concat_axis=0, tiled=True)

    ids = route_ids.T
    wts = route_weights.T
    experts = lax.broadcasted_iota(jnp.int32, (n_ep, tok), 0)
    picks = [ids[k][None, :] == experts for k in range(top)]
    named = picks[0] | picks[1]
    earlier = (
        lax.broadcasted_iota(jnp.int32, (tok, tok), 0)
        < lax.broadcasted_iota(jnp.int32, (tok, tok), 1)
    ).astype(BF16)
    rank = mm(named.astype(BF16), earlier).astype(jnp.int32)
    key = jnp.where(named, rank, -1)
    hit = key[:, None, :] == lax.broadcasted_iota(jnp.int32, (n_ep, cap, tok), 1)
    place = hit.astype(BF16).reshape(slots, tok)
    share = jnp.where(picks[0], wts[0][None, :], 0) + jnp.where(picks[1], wts[1][None, :], 0)
    place_w = jnp.where(hit, share.astype(BF16)[:, None, :], 0).astype(BF16).reshape(slots, tok)

    full = cap + thin
    key_more = jnp.concatenate(
        [key, lax.broadcasted_iota(jnp.int32, (n_ep, thin), 1) + cap], axis=1
    )
    hit_more = key_more[:, None, :] == lax.broadcasted_iota(
        jnp.int32, (n_ep, full, tok + thin), 1
    )
    mine = jnp.concatenate([dense_in, dense_out], axis=1)
    rows = jnp.concatenate([cols(tokens, own), mine], axis=0)
    x_send = mm(hit_more.astype(BF16).reshape(n_ep * full, tok + thin), rows)
    x_send = x_send.astype(BF16).reshape(n_ep, full, quarter)
    x_all = exchange(x_send)
    gate_w, up_w, down_w = w_gate[0], w_up[0], w_down[0]
    x_all, gate_t, up_t, down_t = lax.optimization_barrier(
        (x_all, gate_w.T, up_w.T, down_w.T)
    )
    y_pair = jnp.concatenate([cols(cotangent, own), cols(cotangent, nxt)], axis=1)
    y_send = mm(place_w, y_pair).astype(BF16).reshape(n_ep, cap, 2 * quarter)
    f_send = mm(place, cols(tokens, far)).astype(BF16).reshape(n_ep, cap, quarter)

    def owned(a):
        return lax.dynamic_index_in_dim(
            a.reshape(tok, n_ep, n_tp, thin), own, 2, keepdims=False
        ).reshape(tok, n_ep * thin)

    tokens_own, cot_own = owned(tokens), owned(cotangent)
    f_send, tokens_own, cot_own = lax.optimization_barrier((f_send, tokens_own, cot_own))
    y_got = exchange(y_send).reshape(slots, 2 * quarter)
    x_far = exchange(f_send).reshape(slots, quarter)
    x_all_up = lax.ppermute(x_all, "tp", up)
    x_all_dn = lax.ppermute(x_all, "tp", down)
    x_own = x_all[:, :cap].reshape(slots, quarter)
    x_prv, x_nxt = [a[:, :cap].reshape(slots, quarter) for a in (x_all_up, x_all_dn)]
    d_own, d_prv, d_nxt = [a[:, cap:] for a in (x_all, x_all_up, x_all_dn)]
    d_far_low = lax.ppermute(d_prv[n_ep // 2 :], "tp", up)
    d_far_top = lax.ppermute(d_nxt[: n_ep // 2], "tp", down)
    y_own, y_nxt = y_got[:, :quarter], y_got[:, quarter:]
    y_prv = lax.ppermute(y_own, "tp", up)
    y_far = lax.ppermute(y_nxt, "tp", down)

    tile = slots // TILES

    def by_tile(a):
        return a, pl.BlockSpec((tile, a.shape[1]), lambda t, q: (t, 0))

    def by_row(a, k):
        return a, pl.BlockSpec((quarter, hid), lambda t, q: (q[k], 0))

    def by_col(a, k):
        return a, pl.BlockSpec((hid, quarter), lambda t, q: (0, q[k]))

    def whole(a):
        return a, pl.BlockSpec(a.shape, lambda t, q: (0, 0))

    def wide(width_, dtype):
        return by_tile(jax.ShapeDtypeStruct((slots, width_), dtype))

    unit = 2 * slots * quarter * hid
    parts = call(
        first_parts,
        TILES,
        q,
        [by_tile(a) for a in (x_own, x_nxt, x_prv, y_own, y_nxt)]
        + [by_row(gate_w, k) for k in range(3)]
        + [by_row(up_w, k) for k in range(3)]
        + [by_row(down_t, k) for k in range(2)],
        [wide(hid, F32)] * 3,
        8 * unit,
    )
    act, d_gate, d_up, w_part, mid, ahead, behind, away = call(
        last_parts,
        TILES,
        q,
        [by_tile(a) for a in (*parts, x_far, y_prv, y_far)]
        + [by_row(gate_w, 3), by_row(up_w, 3), by_row(down_t, 2), by_row(down_t, 3)]
        + [by_col(gate_t, k) for k in range(4)]
        + [by_col(up_t, k) for k in range(4)],
        [wide(hid, BF16)] * 3 + [wide(1, F32)] + [wide(quarter, BF16)] * 4,
        12 * unit,
    )
    ahead = lax.ppermute(ahead, "tp", up)
    behind = lax.ppermute(behind, "tp", down)

    def placed(size):
        at = lax.broadcasted_iota(jnp.int32, (n_ep, size, tok), 1)
        return (key[:, None, :] == at).astype(BF16).reshape(n_ep * size, tok)

    w_rows = w_part.reshape(n_ep, 1, cap)
    w_high = w_rows.astype(BF16)
    w_low = (w_rows - w_high.astype(F32)).astype(BF16)

    def line(a):
        return jnp.pad(a.astype(BF16), ((0, 0), (0, 0), (0, quarter - a.shape[2])))

    lines = jnp.pad(jnp.concatenate([line(w_high), line(w_low)], axis=1), ((0, 0), (0, 6), (0, 0)))
    p_send = jnp.concatenate([away.reshape(n_ep, cap, quarter), lines], axis=1)
    p_got = exchange(p_send)
    w_back = p_got[:, cap, :cap].astype(F32) + p_got[:, cap + 1, :cap].astype(F32)
    from_far = mm(placed(cap + 8), p_got.reshape(n_ep * (cap + 8), quarter), ROWS).astype(BF16)
    from_far = lax.ppermute(from_far, "tp", [(k, k ^ 2) for k in range(n_tp)])

    grad_gate, grad_up, grad_down = call(
        weight_grads,
        n_tp,
        q,
        [whole(a) for a in (x_own, x_nxt, x_prv, x_far, y_own, y_nxt, y_prv, y_far)]
        + [whole(d_gate), whole(d_up), whole(act)],
        [
            (jax.ShapeDtypeStruct((width, hid), F32), pl.BlockSpec((quarter, hid), lambda t, q: (q[t], 0))),
            (jax.ShapeDtypeStruct((width, hid), F32), pl.BlockSpec((quarter, hid), lambda t, q: (q[t], 0))),
            (jax.ShapeDtypeStruct((hid, width), F32), pl.BlockSpec((hid, quarter), lambda t, q: (0, q[t]))),
        ],
        12 * unit,
    )

    d_far = jnp.concatenate([d_far_top, d_far_low], axis=0)
    both = jnp.zeros((n_ep, n_tp, thin, 2 * hidden), BF16)
    for piece, k in ((d_own, own), (d_nxt, nxt), (d_prv, prv), (d_far, far)):
        both = lax.dynamic_update_index_in_dim(both, piece, k, 1)
    both = both.reshape(width, 2 * hidden)
    in_whole, out_whole = both[:, :hidden], both[:, hidden:]
    dense_pre = mm(tokens, in_whole)
    dense_act = jax.nn.silu(dense_pre).astype(BF16)
    mix = jax.nn.sigmoid(jnp.dot(tokens, dense_gate, preferred_element_type=F32))
    dense_scaled = (mix[:, None] * cotangent.astype(F32)).astype(BF16)
    cot_out = mm(cotangent, out_whole)
    dense_back = mm(dense_scaled, out_whole)
    sig_pre = jax.nn.sigmoid(dense_pre)
    dense_dpre = (dense_back * sig_pre * (1.0 + dense_pre * (1.0 - sig_pre))).astype(BF16)
    dlogit = mix * (1.0 - mix) * jnp.sum(dense_act.astype(F32) * cot_out, axis=1)
    in_rows = lax.dynamic_slice_in_dim(in_whole, own * quarter, quarter, 0)
    dense_dx = mm(dense_dpre, in_rows, COLS)
    gate_cols = lax.dynamic_slice_in_dim(dense_gate, own * quarter, quarter, 0)
    dense_dx = dense_dx + dlogit[:, None] * gate_cols.astype(F32)[None, :]

    in_part = mm(tokens_own, dense_dpre, ROWS)
    scaled_own = (mix[:, None] * cot_own.astype(F32)).astype(BF16)
    out_part = mm(scaled_own, dense_act, ROWS)
    gate_part = jnp.sum(tokens_own.astype(F32) * dlogit[:, None], axis=0)
    sent = jnp.concatenate([in_part, out_part], axis=1).reshape(n_ep, thin, 2 * hidden)
    tail = jnp.pad(line(gate_part.reshape(n_ep, 1, thin)), ((0, 0), (0, 7), (0, 0)))
    sent = jnp.concatenate([sent.astype(BF16), tail], axis=1)
    total = (mid.astype(F32) + ahead.astype(F32) + behind.astype(F32)).astype(BF16)
    r_send = jnp.concatenate([total.reshape(n_ep, cap, quarter), sent], axis=1)
    r_got = exchange(r_send)
    summed = jnp.sum(r_got[:, cap:].astype(F32), axis=0)
    w_back = w_back + lax.ppermute(w_back, "tp", [(k, k ^ 1) for k in range(n_tp)])
    w_back = w_back + lax.ppermute(w_back, "tp", [(k, k ^ 2) for k in range(n_tp)])
    per_expert = jnp.sum(jnp.where(hit, w_back[:, :, None], 0.0), axis=1)
    grad_route_weights = jnp.stack(
        [
            jnp.sum(jnp.where(picks[k], per_expert, 0.0), axis=0) / wts[k].astype(F32)
            for k in range(top)
        ],
        axis=1,
    ).astype(BF16)
    deep = r_got.shape[1]
    from_own = mm(placed(deep), r_got.reshape(n_ep * deep, quarter), ROWS)
    grad_tokens = (dense_dx + from_own + from_far.astype(F32)).astype(BF16)
    return (
        grad_tokens,
        grad_route_weights,
        grad_gate[None],
        grad_up[None],
        grad_down[None],
        summed[:thin, :hidden],
        summed[:thin, hidden:],
        summed[thin, :thin],
    )


def solution(mesh):
    both = ("ep", "tp")

    return jax.shard_map(
        shards,
        mesh=mesh,
        in_specs=(
            P("ep", None),
            P("ep", None),
            P("ep", None),
            P("ep", None),
            P("ep", None, "tp"),
            P("ep", None, "tp"),
            P("ep", "tp", None),
            P(both, None),
            P(both, None),
            P(),
        ),
        out_specs=(
            P("ep", "tp"),
            P("ep", None),
            P("ep", None, "tp"),
            P("ep", None, "tp"),
            P("ep", "tp", None),
            P(both, None),
            P(both, None),
            P(both),
        ),
        check_vma=False,
    )
```

```python
import jax
import jax.numpy as jnp
from jax import lax
from jax.experimental import pallas as pl
from jax.experimental.pallas import tpu as pltpu
from jax.sharding import PartitionSpec as P


CLAMP_LIMIT = 7.0
SIG_SLOPE = 1.702
F32 = jnp.float32
BF16 = jnp.bfloat16
PLAIN = (((1,), (0,)), ((), ()))
COLS = (((1,), (1,)), ((), ()))
ROWS = (((0,), (0,)), ((), ()))
TILES = 4


def mm(a, b, dims=PLAIN):
    return lax.dot_general(a, b, dims, preferred_element_type=F32)


def call(body, grid, q, ins, outs, flops):
    nbytes = sum(a.size * a.dtype.itemsize for a, _ in ins)
    nbytes += sum(a.size * a.dtype.itemsize for a, _ in outs)
    return pl.pallas_call(
        body,
        grid_spec=pltpu.PrefetchScalarGridSpec(
            num_scalar_prefetch=1,
            grid=(grid,),
            in_specs=[spec for _, spec in ins],
            out_specs=[spec for _, spec in outs],
        ),
        out_shape=[a for a, _ in outs],
        cost_estimate=pl.CostEstimate(flops=flops, bytes_accessed=nbytes, transcendentals=0),
    )(q, *[a for a, _ in ins])


def first_parts(q, xa, xn, xp, ya, yb, ga, gn, gp, ua, un, up, da, dn, gate_o, up_o, back_o):
    gate_o[...] = mm(xa[...], ga[...]) + mm(xn[...], gn[...]) + mm(xp[...], gp[...])
    up_o[...] = mm(xa[...], ua[...]) + mm(xn[...], un[...]) + mm(xp[...], up[...])
    back_o[...] = mm(ya[...], da[...]) + mm(yb[...], dn[...])


def last_parts(
    q, gate_in, up_in, back_in, xf, yp, yf, gf, uf, dp, df, *more
):
    turned, (act_o, dgate_o, dup_o, w_o, *parts_o) = more[:6], more[6:]
    gate_pre = gate_in[...] + mm(xf[...], gf[...])
    up_pre = up_in[...] + mm(xf[...], uf[...])
    gate_clamp = jnp.minimum(gate_pre, CLAMP_LIMIT)
    up_clamp = jnp.clip(up_pre, -CLAMP_LIMIT, CLAMP_LIMIT)
    sig = jax.nn.sigmoid(SIG_SLOPE * gate_clamp)
    glu = gate_clamp * sig
    act = (glu * (up_clamp + 1.0)).astype(BF16)
    act_o[...] = act
    back = back_in[...] + mm(yp[...], dp[...]) + mm(yf[...], df[...])
    w_o[...] = jnp.sum(act.astype(F32) * back, axis=1, keepdims=True)
    slope = (up_clamp + 1.0) * (sig + SIG_SLOPE * gate_clamp * sig * (1.0 - sig))
    d_gate = jnp.where(gate_pre < CLAMP_LIMIT, back * slope, 0.0).astype(BF16)
    d_up = jnp.where(jnp.abs(up_pre) < CLAMP_LIMIT, back * glu, 0.0).astype(BF16)
    dgate_o[...] = d_gate
    dup_o[...] = d_up
    for k, out in enumerate(parts_o):
        out[...] = (mm(d_gate, turned[k][...]) + mm(d_up, turned[3 + k][...])).astype(BF16)


def own_part(q, dg, du, ga, ua, out):
    out[...] = (mm(dg[...], ga[...]) + mm(du[...], ua[...])).astype(BF16)


def weight_grads(q, xa, xn, xp, xf, ya, yn, yp, yf, dg, du, act, gate_o, up_o, down_o):
    for k, (x, y) in enumerate(((xa, ya), (xn, yn), (xp, yp), (xf, yf))):

        @pl.when(pl.program_id(0) == k)
        def _():
            gate_o[...] = mm(x[...], dg[...], ROWS)
            up_o[...] = mm(x[...], du[...], ROWS)
            down_o[...] = mm(act[...], y[...], ROWS)


def shards(
    tokens,
    cotangent,
    route_ids,
    route_weights,
    w_gate,
    w_up,
    w_down,
    dense_in,
    dense_out,
    dense_gate,
):
    n_ep = lax.axis_size("ep")
    n_tp = lax.axis_size("tp")
    tp = lax.axis_index("tp")
    tok, width = tokens.shape
    top = route_ids.shape[1]
    cap = 2 * tok * top // n_ep
    slots = n_ep * cap
    quarter = width // n_tp
    hid = w_gate.shape[2]
    thin, hidden = dense_in.shape
    up = [(k, (k + 1) % n_tp) for k in range(n_tp)]
    down = [(k, (k - 1) % n_tp) for k in range(n_tp)]
    own, nxt, prv, far = tp, (tp + 1) % n_tp, (tp + 3) % n_tp, (tp + 2) % n_tp
    q = jnp.stack([own, nxt, prv, far]).astype(jnp.int32)

    def cols(a, k):
        return lax.dynamic_slice_in_dim(a, k * quarter, quarter, 1)

    def exchange(a):
        return lax.all_to_all(a, "ep", split_axis=0, concat_axis=0, tiled=True)

    ids = route_ids.T
    wts = route_weights.T
    experts = lax.broadcasted_iota(jnp.int32, (n_ep, tok), 0)
    picks = [ids[k][None, :] == experts for k in range(top)]
    named = picks[0] | picks[1]
    earlier = (
        lax.broadcasted_iota(jnp.int32, (tok, tok), 0)
        < lax.broadcasted_iota(jnp.int32, (tok, tok), 1)
    ).astype(BF16)
    rank = mm(named.astype(BF16), earlier).astype(jnp.int32)
    key = jnp.where(named, rank, -1)
    hit = key[:, None, :] == lax.broadcasted_iota(jnp.int32, (n_ep, cap, tok), 1)
    place = hit.astype(BF16).reshape(slots, tok)
    share = jnp.where(picks[0], wts[0][None, :], 0) + jnp.where(picks[1], wts[1][None, :], 0)
    place_w = jnp.where(hit, share.astype(BF16)[:, None, :], 0).astype(BF16).reshape(slots, tok)

    full = cap + thin
    key_more = jnp.concatenate(
        [key, lax.broadcasted_iota(jnp.int32, (n_ep, thin), 1) + cap], axis=1
    )
    hit_more = key_more[:, None, :] == lax.broadcasted_iota(
        jnp.int32, (n_ep, full, tok + thin), 1
    )
    mine = jnp.concatenate([dense_in, dense_out], axis=1)
    rows = jnp.concatenate([cols(tokens, own), mine], axis=0)
    x_send = mm(hit_more.astype(BF16).reshape(n_ep * full, tok + thin), rows)
    x_send = x_send.astype(BF16).reshape(n_ep, full, quarter)
    x_all = exchange(x_send)
    gate_w, up_w, down_w = w_gate[0], w_up[0], w_down[0]
    x_all, gate_t, up_t, down_t = lax.optimization_barrier(
        (x_all, gate_w.T, up_w.T, down_w.T)
    )
    y_pair = jnp.concatenate([cols(cotangent, own), cols(cotangent, nxt)], axis=1)
    y_send = mm(place_w, y_pair).astype(BF16).reshape(n_ep, cap, 2 * quarter)
    f_send = mm(place, cols(tokens, far)).astype(BF16).reshape(n_ep, cap, quarter)

    def owned(a):
        return lax.dynamic_index_in_dim(
            a.reshape(tok, n_ep, n_tp, thin), own, 2, keepdims=False
        ).reshape(tok, n_ep * thin)

    tokens_own, cot_own = owned(tokens), owned(cotangent)
    f_send, tokens_own, cot_own = lax.optimization_barrier((f_send, tokens_own, cot_own))
    y_got = exchange(y_send).reshape(slots, 2 * quarter)
    x_far = exchange(f_send).reshape(slots, quarter)
    x_all_up = lax.ppermute(x_all, "tp", up)
    x_all_dn = lax.ppermute(x_all, "tp", down)
    x_own = x_all[:, :cap].reshape(slots, quarter)
    x_prv, x_nxt = [a[:, :cap].reshape(slots, quarter) for a in (x_all_up, x_all_dn)]
    d_own, d_prv, d_nxt = [a[:, cap:] for a in (x_all, x_all_up, x_all_dn)]
    d_far_low = lax.ppermute(d_prv[n_ep // 2 :], "tp", up)
    d_far_top = lax.ppermute(d_nxt[: n_ep // 2], "tp", down)
    y_own, y_nxt = y_got[:, :quarter], y_got[:, quarter:]
    y_prv = lax.ppermute(y_own, "tp", up)
    y_far = lax.ppermute(y_nxt, "tp", down)

    tile = slots // TILES

    def by_tile(a):
        return a, pl.BlockSpec((tile, a.shape[1]), lambda t, q: (t, 0))

    def by_row(a, k):
        return a, pl.BlockSpec((quarter, hid), lambda t, q: (q[k], 0))

    def by_col(a, k):
        return a, pl.BlockSpec((hid, quarter), lambda t, q: (0, q[k]))

    def whole(a):
        return a, pl.BlockSpec(a.shape, lambda t, q: (0, 0))

    def wide(width_, dtype):
        return by_tile(jax.ShapeDtypeStruct((slots, width_), dtype))

    unit = 2 * slots * quarter * hid
    parts = call(
        first_parts,
        TILES,
        q,
        [by_tile(a) for a in (x_own, x_nxt, x_prv, y_own, y_nxt)]
        + [by_row(gate_w, k) for k in range(3)]
        + [by_row(up_w, k) for k in range(3)]
        + [by_row(down_t, k) for k in range(2)],
        [wide(hid, F32)] * 3,
        8 * unit,
    )
    act, d_gate, d_up, w_part, ahead, behind, away = call(
        last_parts,
        TILES,
        q,
        [by_tile(a) for a in (*parts, x_far, y_prv, y_far)]
        + [by_row(gate_w, 3), by_row(up_w, 3), by_row(down_t, 2), by_row(down_t, 3)]
        + [by_col(gate_t, k) for k in range(1, 4)]
        + [by_col(up_t, k) for k in range(1, 4)],
        [wide(hid, BF16)] * 3 + [wide(1, F32)] + [wide(quarter, BF16)] * 3,
        10 * unit,
    )
    ahead = lax.ppermute(ahead, "tp", up)
    behind = lax.ppermute(behind, "tp", down)

    def placed(size):
        at = lax.broadcasted_iota(jnp.int32, (n_ep, size, tok), 1)
        return (key[:, None, :] == at).astype(BF16).reshape(n_ep * size, tok)

    w_rows = w_part.reshape(n_ep, 1, cap)
    w_high = w_rows.astype(BF16)
    w_low = (w_rows - w_high.astype(F32)).astype(BF16)

    def line(a):
        return jnp.pad(a.astype(BF16), ((0, 0), (0, 0), (0, quarter - a.shape[2])))

    lines = jnp.pad(jnp.concatenate([line(w_high), line(w_low)], axis=1), ((0, 0), (0, 6), (0, 0)))
    p_send = jnp.concatenate([away.reshape(n_ep, cap, quarter), lines], axis=1)
    p_got = exchange(p_send)
    w_back = p_got[:, cap, :cap].astype(F32) + p_got[:, cap + 1, :cap].astype(F32)
    from_far = mm(placed(cap + 8), p_got.reshape(n_ep * (cap + 8), quarter), ROWS).astype(BF16)
    from_far = lax.ppermute(from_far, "tp", [(k, k ^ 2) for k in range(n_tp)])

    grad_gate, grad_up, grad_down = call(
        weight_grads,
        n_tp,
        q,
        [whole(a) for a in (x_own, x_nxt, x_prv, x_far, y_own, y_nxt, y_prv, y_far)]
        + [whole(d_gate), whole(d_up), whole(act)],
        [
            (jax.ShapeDtypeStruct((width, hid), F32), pl.BlockSpec((quarter, hid), lambda t, q: (q[t], 0))),
            (jax.ShapeDtypeStruct((width, hid), F32), pl.BlockSpec((quarter, hid), lambda t, q: (q[t], 0))),
            (jax.ShapeDtypeStruct((hid, width), F32), pl.BlockSpec((hid, quarter), lambda t, q: (0, q[t]))),
        ],
        12 * unit,
    )

    d_far = jnp.concatenate([d_far_top, d_far_low], axis=0)
    both = jnp.zeros((n_ep, n_tp, thin, 2 * hidden), BF16)
    for piece, k in ((d_own, own), (d_nxt, nxt), (d_prv, prv), (d_far, far)):
        both = lax.dynamic_update_index_in_dim(both, piece, k, 1)
    both = both.reshape(width, 2 * hidden)
    in_whole, out_whole = both[:, :hidden], both[:, hidden:]
    dense_pre = mm(tokens, in_whole)
    dense_act = jax.nn.silu(dense_pre).astype(BF16)
    mix = jax.nn.sigmoid(jnp.dot(tokens, dense_gate, preferred_element_type=F32))
    dense_scaled = (mix[:, None] * cotangent.astype(F32)).astype(BF16)
    cot_out = mm(cotangent, out_whole)
    dense_back = mm(dense_scaled, out_whole)
    sig_pre = jax.nn.sigmoid(dense_pre)
    dense_dpre = (dense_back * sig_pre * (1.0 + dense_pre * (1.0 - sig_pre))).astype(BF16)
    dlogit = mix * (1.0 - mix) * jnp.sum(dense_act.astype(F32) * cot_out, axis=1)
    in_rows = lax.dynamic_slice_in_dim(in_whole, own * quarter, quarter, 0)
    dense_dx = mm(dense_dpre, in_rows, COLS)
    gate_cols = lax.dynamic_slice_in_dim(dense_gate, own * quarter, quarter, 0)
    dense_dx = dense_dx + dlogit[:, None] * gate_cols.astype(F32)[None, :]

    in_part = mm(tokens_own, dense_dpre, ROWS)
    scaled_own = (mix[:, None] * cot_own.astype(F32)).astype(BF16)
    out_part = mm(scaled_own, dense_act, ROWS)
    gate_part = jnp.sum(tokens_own.astype(F32) * dlogit[:, None], axis=0)
    sent = jnp.concatenate([in_part, out_part], axis=1).reshape(n_ep, thin, 2 * hidden)
    tail = jnp.pad(line(gate_part.reshape(n_ep, 1, thin)), ((0, 0), (0, 7), (0, 0)))
    sent = jnp.concatenate([sent.astype(BF16), tail], axis=1)
    (mid,) = call(
        own_part,
        TILES,
        q,
        [by_tile(d_gate), by_tile(d_up), by_col(gate_t, 0), by_col(up_t, 0)],
        [wide(quarter, BF16)],
        2 * unit,
    )
    total = (mid.astype(F32) + ahead.astype(F32) + behind.astype(F32)).astype(BF16)
    r_send = jnp.concatenate([total.reshape(n_ep, cap, quarter), sent], axis=1)
    r_got = exchange(r_send)
    summed = jnp.sum(r_got[:, cap:].astype(F32), axis=0)
    w_back = w_back + lax.ppermute(w_back, "tp", [(k, k ^ 1) for k in range(n_tp)])
    w_back = w_back + lax.ppermute(w_back, "tp", [(k, k ^ 2) for k in range(n_tp)])
    per_expert = jnp.sum(jnp.where(hit, w_back[:, :, None], 0.0), axis=1)
    grad_route_weights = jnp.stack(
        [
            jnp.sum(jnp.where(picks[k], per_expert, 0.0), axis=0) / wts[k].astype(F32)
            for k in range(top)
        ],
        axis=1,
    ).astype(BF16)
    deep = r_got.shape[1]
    from_own = mm(placed(deep), r_got.reshape(n_ep * deep, quarter), ROWS)
    grad_tokens = (dense_dx + from_own + from_far.astype(F32)).astype(BF16)
    return (
        grad_tokens,
        grad_route_weights,
        grad_gate[None],
        grad_up[None],
        grad_down[None],
        summed[:thin, :hidden],
        summed[:thin, hidden:],
        summed[thin, :thin],
    )


def solution(mesh):
    both = ("ep", "tp")

    return jax.shard_map(
        shards,
        mesh=mesh,
        in_specs=(
            P("ep", None),
            P("ep", None),
            P("ep", None),
            P("ep", None),
            P("ep", None, "tp"),
            P("ep", None, "tp"),
            P("ep", "tp", None),
            P(both, None),
            P(both, None),
            P(),
        ),
        out_specs=(
            P("ep", "tp"),
            P("ep", None),
            P("ep", None, "tp"),
            P("ep", None, "tp"),
            P("ep", "tp", None),
            P(both, None),
            P(both, None),
            P(both),
        ),
        check_vma=False,
    )
```
